32 devices in a mesh: fs: 8 (over z, y), tp: 4 (over x, core).
Axes of the slice: x: 2, y: 2, z: 4, core: 2. Of those that a mesh axis runs over, the one named last changes fastest.
Arguments:
- tokens: bfloat16 [8192, 2048], P('fs'), may hold values from -6 to 6
- norm_gain: float32 [2048], replicated, may hold values from 0.1 to 1.9
- gate_weight: bfloat16 [2048, 5632], P('fs', 'tp'), may hold values from -0.125 to 0.125
- up_weight: bfloat16 [2048, 5632], P('fs', 'tp'), may hold values from -0.125 to 0.125
- down_weight: bfloat16 [5632, 2048], P('tp', 'fs'), may hold values from -0.078125 to 0.078125
Outputs:
- mixed: bfloat16 [8192, 2048], P(('fs', 'tp'))
The draws below stay inside these ranges and needn't reach their ends.
All inputs are finite; a program needn't handle non-finite values.
Results may differ from the reference program's by a relative error of at most 0.014.
Values may be sent and summed in bfloat16 or wider, within the bound.
A program may use at most 128 MiB of HBM per device.

```python
import jax
import jax.numpy as jnp
from jax import lax

D = 2048
FF = 5632
TOKENS = 8192
N_FS = 8
N_TP = 4


def block_scale(own_key, extent, cuts, low, high):
    loudness = 1.0
    for axis_at, blocks in cuts:
        heights = jax.random.uniform(jax.random.fold_in(jax.random.fold_in(own_key, 6), axis_at), (blocks,), jnp.float32, low / len(cuts), high / len(cuts))
        loudness = loudness * jnp.repeat(jnp.exp(heights), extent[axis_at] // blocks).reshape((-1,) + (1,) * (len(extent) - 1 - axis_at))
    return loudness


def gaussian(key, dims, spread, limit, shards=(), kind=jnp.bfloat16):
    values = jax.random.normal(key, dims, jnp.float32) * spread
    if len(shards) > 0:
        values = block_scale(key, dims, shards, -0.22, 0.18) * values
    return jnp.clip(values, min=-limit, max=limit).astype(kind)


def setup_inputs(seed: int = 0) -> dict:
    splits = jax.random.split(jax.random.key(seed), 6)
    tokens = gaussian(splits[0], (TOKENS, D), 1.0, 6.0, ((0, 8),))
    norm_gain = jnp.clip(1.0 + 0.18 * jax.random.normal(splits[1], (D,), jnp.float32), 0.1, 1.9)
    gate_weight = gaussian(splits[2], (D, FF), D ** -0.5, 0.125, ((0, 8), (1, 4)))
    up_weight = gaussian(splits[3], (D, FF), D ** -0.5, 0.125, ((0, 8), (1, 4)))
    down_weight = gaussian(splits[4], (FF, D), FF ** -0.5, 0.078125, ((0, 4), (1, 8)))
    return {"tokens": tokens, "norm_gain": norm_gain, "gate_weight": gate_weight, "up_weight": up_weight, "down_weight": down_weight}


def block_rows(xrows, norm_gain, gate_weight, up_weight, down_weight):
    xf = xrows.astype(jnp.float32)
    scale = lax.rsqrt(lax.optimization_barrier(jnp.mean(xf * xf, axis=-1, keepdims=True)) + 1e-06)
    normed = (xf * scale * norm_gain).astype(jnp.bfloat16)
    gate = jnp.dot(normed, gate_weight, preferred_element_type=jnp.float32)
    up = jnp.dot(normed, up_weight, preferred_element_type=jnp.float32)
    hidden = (jax.nn.silu(gate) * up).astype(jnp.bfloat16)
    width = FF // N_TP

    def add_block(total, index):
        start = (index * width).astype(jnp.int32)
        left = lax.dynamic_slice_in_dim(hidden, start, width, 1)
        right = lax.dynamic_slice_in_dim(down_weight, start, width, 0)
        part = jnp.dot(left, right, preferred_element_type=jnp.float32).astype(jnp.bfloat16)
        return (total + part.astype(jnp.float32), None)
    total, unused = lax.scan(add_block, jnp.zeros((xrows.shape[0], D), jnp.float32), jnp.arange(N_TP, dtype=jnp.int32))
    return total.astype(jnp.bfloat16)

def reference(tokens, norm_gain, gate_weight, up_weight, down_weight):
    blocks = tokens.reshape(N_FS, TOKENS // N_FS, D)
    result = lax.map(lambda rows: block_rows(rows, norm_gain, gate_weight, up_weight, down_weight), blocks)
    return result.reshape(TOKENS, D)
```

```python
import jax
import jax.numpy as jnp
from jax import lax
from jax.sharding import PartitionSpec as P


def ring_order(n):
    ny = 1
    while ny * ny * 4 <= n:
        ny *= 2
    nz = n // ny
    if ny == 1 or nz == 1 or ny % 2:
        return list(range(n))
    cells = []
    for y in range(ny):
        column = list(range(1, nz))
        cells += [(z, y) for z in (column if y % 2 == 0 else column[::-1])]
    cells += [(0, y) for y in reversed(range(ny))]
    return [z * ny + y for z, y in cells]


def make_per_device(n, n_tp):
    order = ring_order(n)
    place = [order.index(i) for i in range(n)]
    right = [(order[i], order[(i + 1) % n]) for i in range(n)]
    left = [(order[i], order[(i - 1) % n]) for i in range(n)]

    def per_device(tokens, norm_gain, gate_weight, up_weight, down_weight):
        rows = gate_weight.shape[0]
        wide = down_weight.shape[1]
        at = jnp.asarray(place, jnp.int32)[lax.axis_index("fs")]
        ring = jnp.asarray(order, jnp.int32)
        mine = lax.axis_index("tp")

        def owner(step):
            return ring[(at - step + n) % n]

        xf = tokens.astype(jnp.float32)
        scale = lax.rsqrt(jnp.mean(xf * xf, axis=-1, keepdims=True) + 1e-06)
        normed = (xf * scale * norm_gain).astype(jnp.bfloat16)

        def product(step, block):
            part = lax.dynamic_slice_in_dim(normed, owner(step) * rows, rows, 1)
            return jnp.dot(part, block, preferred_element_type=jnp.float32)

        g, u, d = gate_weight, up_weight, down_weight
        gate = up = None
        for step in range(1, n + 1):
            if step < n:
                g_next = lax.ppermute(g, "fs", right)
                u_next = lax.ppermute(u, "fs", left)
            g_part, u_part = product(step - 1, g), product(1 - step, u)
            gate = g_part if gate is None else gate + g_part
            up = u_part if up is None else up + u_part
            if step < n - 1:
                g, u, gate, up = lax.optimization_barrier((g_next, u_next, gate, up))
            elif step == n - 1:
                g, u = g_next, u_next
            if step == n - 2:
                g, u, d = lax.optimization_barrier((g, u, d))
        hidden = (jax.nn.silu(gate) * up).astype(jnp.bfloat16)

        keep = tokens.shape[0] // n_tp
        out = jnp.zeros((keep, wide * n), jnp.bfloat16)

        def finish(out, steps, blocks):
            terms = [jnp.dot(hidden, b, preferred_element_type=jnp.float32).astype(jnp.bfloat16) for b in blocks]
            terms = jnp.concatenate(terms, axis=1) if len(terms) > 1 else terms[0]
            terms = terms.reshape(n_tp, keep, terms.shape[1])
            total = lax.dynamic_index_in_dim(terms, mine, 0, keepdims=False).astype(jnp.float32)
            for shift in range(1, n_tp):
                sent = lax.dynamic_index_in_dim(terms, (mine + shift) % n_tp, 0, keepdims=False)
                got = lax.ppermute(sent, "tp", [(t, (t + shift) % n_tp) for t in range(n_tp)])
                total = total + got.astype(jnp.float32)
            total = total.astype(jnp.bfloat16)
            for i, step in enumerate(steps):
                out = lax.dynamic_update_slice(out, total[:, i * wide : (i + 1) * wide], (0, owner(step) * wide))
            return out

        a, b = d, d
        for step in range(1, n // 2):
            a = lax.ppermute(a, "fs", right)
            b = lax.ppermute(b, "fs", left)
            if step == 1:
                out = finish(out, [0, 1, -1], [d, a, b])
            else:
                out = finish(out, [step, -step], [a, b])
        a = lax.ppermute(a[:, : wide // 2], "fs", right)
        b = lax.ppermute(b[:, wide // 2 :], "fs", left)
        return finish(out, [n // 2], [jnp.concatenate([a, b], axis=1)])

    return per_device


def solution(mesh):
    placed = (P("fs", None), P(), P("fs", "tp"), P("fs", "tp"), P("tp", "fs"))
    return jax.shard_map(
        make_per_device(mesh.shape["fs"], mesh.shape["tp"]),
        mesh=mesh, in_specs=placed, out_specs=P(("fs", "tp"), None), check_vma=False,
    )
```

```python
import functools

import jax
import jax.numpy as jnp
from jax import lax
from jax.experimental import pallas as pl
from jax.experimental.pallas import tpu as pltpu
from jax.sharding import PartitionSpec as P

MESH = pl.DeviceIdType.MESH


def grid_of(n):
    ny = 2
    while ny * ny * 4 <= n:
        ny *= 2
    return n // ny, ny


def fs_of(place, n):
    nz, ny = grid_of(n)
    on = lax.div(place + (n - ny), n)
    rest = (place - ny) * on
    y, r = lax.div(rest, nz - 1), lax.rem(rest, nz - 1)
    odd = lax.rem(y, 2)
    z = 1 + (1 - odd) * r + odd * (nz - 2 - r)
    return on * (z * ny + y) + (1 - on) * (ny - 1 - place)


def place_of(fs, n):
    nz, ny = grid_of(n)
    z, y = lax.div(fs, ny), lax.rem(fs, ny)
    on = lax.div(z + nz - 1, nz)
    up = (z - 1) * on
    odd = lax.rem(y, 2)
    r = (1 - odd) * up + odd * (nz - 2 - up)
    return on * (ny + y * (nz - 1) + r) + (1 - on) * (ny - 1 - y)


def dot(a, b):
    return jnp.dot(a, b, preferred_element_type=jnp.float32)


def kernel(n, n_tp, tokens, gain, gw, uw, dw, out, normed, gacc, uacc, hidden, gbuf, ubuf, dbuf, terms, got,
           send, recv, rs_send, rs_recv, local):
    me, mine = lax.axis_index("fs"), lax.axis_index("tp")
    at = place_of(me, n)
    neighbour = [fs_of(lax.rem(at + 1, n), n), fs_of(lax.rem(at + n - 1, n), n)]
    wide = dw.shape[1]
    rows = gw.shape[0]
    keep = out.shape[0]
    count = normed.shape[0]
    tile = 256

    def owner(way, step):
        step = step if way == 0 else n - step
        return fs_of(lax.rem(at + n - step, n), n)

    barrier = pltpu.get_barrier_semaphore()
    for way in range(2):
        pl.semaphore_signal(barrier, inc=1, device_id={"fs": neighbour[way]}, device_id_type=MESH)
    peers = [lax.rem(mine + k, n_tp) for k in range(1, n_tp)]
    for peer in peers:
        pl.semaphore_signal(barrier, inc=1, device_id={"tp": peer}, device_id_type=MESH)

    loads = [
        pltpu.make_async_copy(tokens, normed, local.at[0]),
        pltpu.make_async_copy(gw, gbuf.at[me], local.at[1]),
        pltpu.make_async_copy(uw, ubuf.at[me], local.at[2]),
        pltpu.make_async_copy(dw, dbuf.at[me], local.at[3]),
    ]
    for load in loads:
        load.start()
    pl.semaphore_wait(barrier, 2 + n_tp - 1)

    def hop(way, own, buf, step, c, event):
        half = own.shape[0] // 2
        part = pl.ds(c * half, half)
        o = owner(way, step)
        return pltpu.make_async_remote_copy(
            src_ref=own.at[part] if step == 0 else buf.at[o, part],
            dst_ref=buf.at[o, part],
            send_sem=send.at[way, event],
            recv_sem=recv.at[way, event],
            device_id={"fs": neighbour[way]},
            device_id_type=MESH,
        )

    def arrive(way, buf, step, c, event):
        half = buf.shape[1] // 2
        here = buf.at[owner(way, step), pl.ds(c * half, half)]
        pltpu.make_async_remote_copy(
            src_ref=here, dst_ref=here, send_sem=send.at[way, event], recv_sem=recv.at[way, event],
            device_id={"fs": neighbour[way]}, device_id_type=MESH,
        ).wait_recv()

    sends = []

    def go(copy):
        copy.start()
        sends.append(copy)

    first = [(gw, gbuf), (uw, ubuf)]
    for c in range(2):
        for way, (own, buf) in enumerate(first):
            go(hop(way, own, buf, 0, c, c))

    loads[0].wait()
    fine = 32

    @pl.loop(0, count // fine)
    def _(i):
        part = pl.ds(pl.multiple_of(i * fine, fine), fine)
        xf = normed[part, :].astype(jnp.float32)
        scale = lax.rsqrt(jnp.mean(xf * xf, axis=-1, keepdims=True) + 1e-06)
        normed[part, :] = (xf * scale * gain[...]).astype(jnp.bfloat16)

    loads[1].wait()
    loads[2].wait()

    def accumulate(step):
        og, ou = owner(0, step), owner(1, step)

        @pl.loop(0, count // tile)
        def _(i):
            part = pl.ds(pl.multiple_of(i * tile, tile), tile)
            for o, buf, acc in ((og, gbuf, gacc), (ou, ubuf, uacc)):
                a = normed[part, pl.ds(pl.multiple_of(o * rows, rows), rows)]
                if step == 0:
                    acc[part, :] = dot(a, buf[o])
                else:
                    acc[part, :] += dot(a, buf[o])

    base = 2 * (n - 1)
    for step in range(1, n):
        for c in range(2):
            for way, (own, buf) in enumerate(first):
                arrive(way, buf, step, c, 2 * (step - 1) + c)
                if step < n - 1:
                    go(hop(way, own, buf, step, c, 2 * step + c))
            if c == 0:
                accumulate(step - 1)
        if step == n - 2:
            for c in range(2):
                for way in range(2):
                    go(hop(way, dw, dbuf, 0, c, base + c))
    accumulate(n - 1)

    @pl.loop(0, count // fine)
    def _(i):
        part = pl.ds(pl.multiple_of(i * fine, fine), fine)
        v = gacc[part, :]
        hidden[part, :] = (v / (1.0 + jnp.exp(-v)) * uacc[part, :]).astype(jnp.bfloat16)

    loads[3].wait()
    shared = []

    def share(o):
        @pl.loop(0, count // tile)
        def _(i):
            part = pl.ds(pl.multiple_of(i * tile, tile), tile)
            terms[o, part, :] = dot(hidden[part, :], dbuf[o]).astype(jnp.bfloat16)

        copies = []
        for k, peer in enumerate(peers):
            copy = pltpu.make_async_remote_copy(
                src_ref=terms.at[o, pl.ds(pl.multiple_of(peer * keep, keep), keep)],
                dst_ref=got.at[k, o],
                send_sem=rs_send.at[len(shared), k],
                recv_sem=rs_recv.at[len(shared), k],
                device_id={"tp": peer},
                device_id_type=MESH,
            )
            go(copy)
            copies.append(copy)
        shared.append((o, copies))

    last = n // 2 - 1
    for step in range(1, n // 2):
        for c in range(2):
            for way in range(2):
                arrive(way, dbuf, step, c, base + 2 * (step - 1) + c)
                if step < last:
                    go(hop(way, dw, dbuf, step, c, base + 2 * step + c))
                elif c == way:
                    go(hop(way, dw, dbuf, step, c, base + 2 * last))
            if step == 1 and c == 0:
                share(me)
        share(owner(0, step))
        share(owner(1, step))
    for way in range(2):
        arrive(way, dbuf, n // 2, way, base + 2 * last)
    share(owner(0, n // 2))

    for o, copies in shared:
        for copy in copies:
            copy.wait_recv()
        total = terms[o, pl.ds(pl.multiple_of(mine * keep, keep), keep), :].astype(jnp.float32)
        for k in range(n_tp - 1):
            total = total + got[k, o].astype(jnp.float32)
        out[:, pl.ds(pl.multiple_of(o * wide, wide), wide)] = total.astype(out.dtype)
    for copy in sends:
        copy.wait_send()


def make_per_device(n, n_tp):
    def per_device(tokens, norm_gain, gate_weight, up_weight, down_weight):
        count, width = tokens.shape
        units = gate_weight.shape[1]
        wide = down_weight.shape[1]
        keep = count // n_tp
        bf16, f32 = jnp.bfloat16, jnp.float32
        events = 2 * (n - 1) + 2 * (n // 2 - 1) + 1
        flops = 6 * count * width * units
        any_ref = pl.BlockSpec(memory_space=pl.ANY)
        vmem_ref = pl.BlockSpec(memory_space=pltpu.VMEM)
        return pl.pallas_call(
            functools.partial(kernel, n, n_tp),
            out_shape=jax.ShapeDtypeStruct((keep, width), bf16),
            in_specs=[any_ref, vmem_ref, any_ref, any_ref, any_ref],
            out_specs=vmem_ref,
            scratch_shapes=[
                pltpu.VMEM((count, width), bf16),
                pltpu.VMEM((count, units), f32),
                pltpu.VMEM((count, units), f32),
                pltpu.VMEM((count, units), bf16),
                pltpu.VMEM((n,) + gate_weight.shape, bf16),
                pltpu.VMEM((n,) + up_weight.shape, bf16),
                pltpu.VMEM((n,) + down_weight.shape, bf16),
                pltpu.VMEM((n, count, wide), bf16),
                pltpu.VMEM((n_tp - 1, n, keep, wide), bf16),
                pltpu.SemaphoreType.DMA((2, events)),
                pltpu.SemaphoreType.DMA((2, events)),
                pltpu.SemaphoreType.DMA((n, n_tp - 1)),
                pltpu.SemaphoreType.DMA((n, n_tp - 1)),
                pltpu.SemaphoreType.DMA((4,)),
            ],
            compiler_params=pltpu.CompilerParams(
                collective_id=0, has_side_effects=True, vmem_limit_bytes=66_000_000
            ),
            cost_estimate=pl.CostEstimate(flops=flops, bytes_accessed=2 * count * width, transcendentals=count * units),
        )(tokens, norm_gain.reshape(1, width), gate_weight, up_weight, down_weight)

    return per_device


def solution(mesh):
    placed = (P("fs", None), P(), P("fs", "tp"), P("fs", "tp"), P("tp", "fs"))
    return jax.shard_map(
        make_per_device(mesh.shape["fs"], mesh.shape["tp"]),
        mesh=mesh, in_specs=placed, out_specs=P(("fs", "tp"), None), check_vma=False,
    )
```

```python
import functools

import jax
import jax.numpy as jnp
from jax import lax
from jax.experimental import pallas as pl
from jax.experimental.pallas import tpu as pltpu
from jax.sharding import PartitionSpec as P

MESH = pl.DeviceIdType.MESH


def grid_of(n):
    ny = 2
    while ny * ny * 4 <= n:
        ny *= 2
    return n // ny, ny


def fs_of(place, n):
    nz, ny = grid_of(n)
    on = lax.div(place + (n - ny), n)
    rest = (place - ny) * on
    y, r = lax.div(rest, nz - 1), lax.rem(rest, nz - 1)
    odd = lax.rem(y, 2)
    z = 1 + (1 - odd) * r + odd * (nz - 2 - r)
    return on * (z * ny + y) + (1 - on) * (ny - 1 - place)


def place_of(fs, n):
    nz, ny = grid_of(n)
    z, y = lax.div(fs, ny), lax.rem(fs, ny)
    on = lax.div(z + nz - 1, nz)
    up = (z - 1) * on
    odd = lax.rem(y, 2)
    r = (1 - odd) * up + odd * (nz - 2 - up)
    return on * (ny + y * (nz - 1) + r) + (1 - on) * (ny - 1 - y)


def dot(a, b):
    return jnp.dot(a, b, preferred_element_type=jnp.float32)


def kernel(n, n_tp, tokens, gain, gw, uw, dw, out, normed, gacc, uacc, hidden, gbuf, ubuf, dbuf, terms, paired, summed,
           got, send, recv, pair_send, pair_recv, rs_send, rs_recv, local):
    me, mine = lax.axis_index("fs"), lax.axis_index("tp")
    at = place_of(me, n)
    neighbour = [fs_of(lax.rem(at + 1, n), n), fs_of(lax.rem(at + n - 1, n), n)]
    wide = dw.shape[1]
    rows = gw.shape[0]
    keep = out.shape[0]
    count = normed.shape[0]
    tile = 256

    def owner(way, step):
        step = step if way == 0 else n - step
        return fs_of(lax.rem(at + n - step, n), n)

    barrier = pltpu.get_barrier_semaphore()
    for way in range(2):
        pl.semaphore_signal(barrier, inc=1, device_id={"fs": neighbour[way]}, device_id_type=MESH)
    chips = n_tp // 2
    core, chip = lax.rem(mine, 2), lax.div(mine, 2)
    partner = 2 * chip + 1 - core
    others = [lax.rem(chip + k, chips) for k in range(1, chips)]
    for peer in [partner] + [2 * other + core for other in others]:
        pl.semaphore_signal(barrier, inc=1, device_id={"tp": peer}, device_id_type=MESH)

    loads = [
        pltpu.make_async_copy(tokens, normed, local.at[0]),
        pltpu.make_async_copy(gw, gbuf.at[me], local.at[1]),
        pltpu.make_async_copy(uw, ubuf.at[me], local.at[2]),
        pltpu.make_async_copy(dw, dbuf.at[me], local.at[3]),
    ]
    for load in loads:
        load.start()
    pl.semaphore_wait(barrier, 2 + chips)

    def hop(way, own, buf, step, c, event):
        half = own.shape[0] // 2
        part = pl.ds(c * half, half)
        o = owner(way, step)
        return pltpu.make_async_remote_copy(
            src_ref=own.at[part] if step == 0 else buf.at[o, part],
            dst_ref=buf.at[o, part],
            send_sem=send.at[way, event],
            recv_sem=recv.at[way, event],
            device_id={"fs": neighbour[way]},
            device_id_type=MESH,
        )

    def arrive(way, buf, step, c, event):
        half = buf.shape[1] // 2
        here = buf.at[owner(way, step), pl.ds(c * half, half)]
        pltpu.make_async_remote_copy(
            src_ref=here, dst_ref=here, send_sem=send.at[way, event], recv_sem=recv.at[way, event],
            device_id={"fs": neighbour[way]}, device_id_type=MESH,
        ).wait_recv()

    sends = []

    def go(copy):
        copy.start()
        sends.append(copy)

    first = [(gw, gbuf), (uw, ubuf)]
    for c in range(2):
        for way, (own, buf) in enumerate(first):
            go(hop(way, own, buf, 0, c, c))

    loads[0].wait()
    fine = 32

    @pl.loop(0, count // fine)
    def _(i):
        part = pl.ds(pl.multiple_of(i * fine, fine), fine)
        xf = normed[part, :].astype(jnp.float32)
        scale = lax.rsqrt(jnp.mean(xf * xf, axis=-1, keepdims=True) + 1e-06)
        normed[part, :] = (xf * scale * gain[...]).astype(jnp.bfloat16)

    loads[1].wait()
    loads[2].wait()

    def accumulate(step):
        og, ou = owner(0, step), owner(1, step)

        @pl.loop(0, count // tile)
        def _(i):
            part = pl.ds(pl.multiple_of(i * tile, tile), tile)
            for o, buf, acc in ((og, gbuf, gacc), (ou, ubuf, uacc)):
                a = normed[part, pl.ds(pl.multiple_of(o * rows, rows), rows)]
                if step == 0:
                    acc[part, :] = dot(a, buf[o])
                else:
                    acc[part, :] += dot(a, buf[o])

    base = 2 * (n - 1)
    for step in range(1, n):
        for c in range(2):
            for way, (own, buf) in enumerate(first):
                arrive(way, buf, step, c, 2 * (step - 1) + c)
                if step < n - 1:
                    go(hop(way, own, buf, step, c, 2 * step + c))
            if c == 0:
                accumulate(step - 1)
        if step == n - 2:
            for c in range(2):
                for way in range(2):
                    go(hop(way, dw, dbuf, 0, c, base + c))
    accumulate(n - 1)

    @pl.loop(0, count // fine)
    def _(i):
        part = pl.ds(pl.multiple_of(i * fine, fine), fine)
        v = gacc[part, :]
        hidden[part, :] = (v / (1.0 + jnp.exp(-v)) * uacc[part, :]).astype(jnp.bfloat16)

    loads[3].wait()
    shared = []

    def kept(index):
        return pl.ds(pl.multiple_of(index * keep, keep), keep)

    def share(o):
        @pl.loop(0, count // tile)
        def _(i):
            part = pl.ds(pl.multiple_of(i * tile, tile), tile)
            terms[o, part, :] = dot(hidden[part, :], dbuf[o]).astype(jnp.bfloat16)

        copies = []
        for k in range(chips):
            to = lax.rem(chip + 1 + k, chips)
            copy = pltpu.make_async_remote_copy(
                src_ref=terms.at[o, kept(2 * to + 1 - core)],
                dst_ref=paired.at[o, k],
                send_sem=pair_send.at[len(shared), k],
                recv_sem=pair_recv.at[len(shared), k],
                device_id={"tp": partner},
                device_id_type=MESH,
            )
            go(copy)
            copies.append(copy)
        shared.append([o, copies, None])

    def cross(j):
        o, pairs, unused = shared[j]
        copies = []
        for k, other in enumerate(others):
            pairs[k].wait_recv()
            total = terms[o, kept(2 * other + core), :].astype(jnp.float32) + paired[o, k].astype(jnp.float32)
            summed[o, k] = total.astype(jnp.bfloat16)
            copy = pltpu.make_async_remote_copy(
                src_ref=summed.at[o, k],
                dst_ref=got.at[k, o],
                send_sem=rs_send.at[j, k],
                recv_sem=rs_recv.at[j, k],
                device_id={"tp": 2 * other + core},
                device_id_type=MESH,
            )
            go(copy)
            copies.append(copy)
        shared[j][2] = copies

    last = n // 2 - 1
    for step in range(1, n // 2):
        for c in range(2):
            for way in range(2):
                arrive(way, dbuf, step, c, base + 2 * (step - 1) + c)
                if step < last:
                    go(hop(way, dw, dbuf, step, c, base + 2 * step + c))
                elif c == way:
                    go(hop(way, dw, dbuf, step, c, base + 2 * last))
            if step == 1 and c == 0:
                share(me)
                cross(0)
        share(owner(0, step))
        share(owner(1, step))
        cross(2 * step - 1)
        cross(2 * step)
    for way in range(2):
        arrive(way, dbuf, n // 2, way, base + 2 * last)
    share(owner(0, n // 2))
    cross(n - 1)

    for o, pairs, copies in shared:
        pairs[chips - 1].wait_recv()
        for copy in copies:
            copy.wait_recv()
        total = terms[o, kept(mine), :].astype(jnp.float32) + paired[o, chips - 1].astype(jnp.float32)
        for k in range(chips - 1):
            total = total + got[k, o].astype(jnp.float32)
        out[:, pl.ds(pl.multiple_of(o * wide, wide), wide)] = total.astype(out.dtype)
    for copy in sends:
        copy.wait_send()


def make_per_device(n, n_tp):
    def per_device(tokens, norm_gain, gate_weight, up_weight, down_weight):
        count, width = tokens.shape
        units = gate_weight.shape[1]
        wide = down_weight.shape[1]
        keep = count // n_tp
        bf16, f32 = jnp.bfloat16, jnp.float32
        events = 2 * (n - 1) + 2 * (n // 2 - 1) + 1
        flops = 6 * count * width * units
        any_ref = pl.BlockSpec(memory_space=pl.ANY)
        vmem_ref = pl.BlockSpec(memory_space=pltpu.VMEM)
        return pl.pallas_call(
            functools.partial(kernel, n, n_tp),
            out_shape=jax.ShapeDtypeStruct((keep, width), bf16),
            in_specs=[any_ref, vmem_ref, any_ref, any_ref, any_ref],
            out_specs=vmem_ref,
            scratch_shapes=[
                pltpu.VMEM((count, width), bf16),
                pltpu.VMEM((count, units), f32),
                pltpu.VMEM((count, units), f32),
                pltpu.VMEM((count, units), bf16),
                pltpu.VMEM((n,) + gate_weight.shape, bf16),
                pltpu.VMEM((n,) + up_weight.shape, bf16),
                pltpu.VMEM((n,) + down_weight.shape, bf16),
                pltpu.VMEM((n, count, wide), bf16),
                pltpu.VMEM((n, n_tp // 2, keep, wide), bf16),
                pltpu.VMEM((n, n_tp // 2 - 1, keep, wide), bf16),
                pltpu.VMEM((n_tp // 2 - 1, n, keep, wide), bf16),
                pltpu.SemaphoreType.DMA((2, events)),
                pltpu.SemaphoreType.DMA((2, events)),
                pltpu.SemaphoreType.DMA((n, n_tp // 2)),
                pltpu.SemaphoreType.DMA((n, n_tp // 2)),
                pltpu.SemaphoreType.DMA((n, n_tp // 2 - 1)),
                pltpu.SemaphoreType.DMA((n, n_tp // 2 - 1)),
                pltpu.SemaphoreType.DMA((4,)),
            ],
            compiler_params=pltpu.CompilerParams(
                collective_id=0, has_side_effects=True, vmem_limit_bytes=66_000_000
            ),
            cost_estimate=pl.CostEstimate(flops=flops, bytes_accessed=2 * count * width, transcendentals=count * units),
        )(tokens, norm_gain.reshape(1, width), gate_weight, up_weight, down_weight)

    return per_device


def solution(mesh):
    placed = (P("fs", None), P(), P("fs", "tp"), P("fs", "tp"), P("tp", "fs"))
    return jax.shard_map(
        make_per_device(mesh.shape["fs"], mesh.shape["tp"]),
        mesh=mesh, in_specs=placed, out_specs=P(("fs", "tp"), None), check_vma=False,
    )
```

```python
import functools

import jax
import jax.numpy as jnp
from jax import lax
from jax.experimental import pallas as pl
from jax.experimental.pallas import tpu as pltpu
from jax.sharding import PartitionSpec as P

MESH = pl.DeviceIdType.MESH


def grid_of(n):
    ny = 2
    while ny * ny * 4 <= n:
        ny *= 2
    return n // ny, ny


def fs_of(place, n):
    nz, ny = grid_of(n)
    on = lax.div(place + (n - ny), n)
    rest = (place - ny) * on
    y, r = lax.div(rest, nz - 1), lax.rem(rest, nz - 1)
    odd = lax.rem(y, 2)
    z = 1 + (1 - odd) * r + odd * (nz - 2 - r)
    return on * (z * ny + y) + (1 - on) * (ny - 1 - place)


def place_of(fs, n):
    nz, ny = grid_of(n)
    z, y = lax.div(fs, ny), lax.rem(fs, ny)
    on = lax.div(z + nz - 1, nz)
    up = (z - 1) * on
    odd = lax.rem(y, 2)
    r = (1 - odd) * up + odd * (nz - 2 - up)
    return on * (ny + y * (nz - 1) + r) + (1 - on) * (ny - 1 - y)


def splits_of(wide):
    return 2 if wide % 256 == 0 else 1


def dot(a, b):
    return jnp.dot(a, b, preferred_element_type=jnp.float32)


def kernel(n, n_tp, tokens, gain, gw, uw, dw, out, normed, gacc, uacc, hidden, gbuf, ubuf, dbuf, terms, paired, summed,
           got, send, recv, pair_send, pair_recv, rs_send, rs_recv, local):
    me, mine = lax.axis_index("fs"), lax.axis_index("tp")
    at = place_of(me, n)
    neighbour = [fs_of(lax.rem(at + 1, n), n), fs_of(lax.rem(at + n - 1, n), n)]
    wide = dw.shape[1]
    rows = gw.shape[0]
    keep = out.shape[0]
    count = normed.shape[0]
    tile = 256

    def owner(way, step):
        step = step if way == 0 else n - step
        return fs_of(lax.rem(at + n - step, n), n)

    barrier = pltpu.get_barrier_semaphore()
    for way in range(2):
        pl.semaphore_signal(barrier, inc=1, device_id={"fs": neighbour[way]}, device_id_type=MESH)
    chips = n_tp // 2
    core, chip = lax.rem(mine, 2), lax.div(mine, 2)
    partner = 2 * chip + 1 - core
    others = [lax.rem(chip + k, chips) for k in range(1, chips)]
    for peer in [partner] + [2 * other + core for other in others]:
        pl.semaphore_signal(barrier, inc=1, device_id={"tp": peer}, device_id_type=MESH)

    loads = [
        pltpu.make_async_copy(tokens, normed, local.at[0]),
        pltpu.make_async_copy(gw, gbuf.at[me], local.at[1]),
        pltpu.make_async_copy(uw, ubuf.at[me], local.at[2]),
        pltpu.make_async_copy(dw, dbuf.at[me], local.at[3]),
    ]
    for load in loads:
        load.start()
    pl.semaphore_wait(barrier, 2 + chips)

    def hop(way, own, buf, step, c, event, cols=None):
        half = own.shape[0] // 2
        part = (pl.ds(c * half, half),) + (() if cols is None else (cols,))
        o = owner(way, step)
        return pltpu.make_async_remote_copy(
            src_ref=own.at[part] if step == 0 else buf.at[(o,) + part],
            dst_ref=buf.at[(o,) + part],
            send_sem=send.at[way, event],
            recv_sem=recv.at[way, event],
            device_id={"fs": neighbour[way]},
            device_id_type=MESH,
        )

    def arrive(way, buf, step, c, event, cols=None):
        half = buf.shape[1] // 2
        part = (pl.ds(c * half, half),) + (() if cols is None else (cols,))
        here = buf.at[(owner(way, step),) + part]
        pltpu.make_async_remote_copy(
            src_ref=here, dst_ref=here, send_sem=send.at[way, event], recv_sem=recv.at[way, event],
            device_id={"fs": neighbour[way]}, device_id_type=MESH,
        ).wait_recv()

    sends = []

    def go(copy):
        copy.start()
        sends.append(copy)

    first = [(gw, gbuf), (uw, ubuf)]
    for c in range(2):
        for way, (own, buf) in enumerate(first):
            go(hop(way, own, buf, 0, c, c))

    loads[0].wait()
    fine = 32

    @pl.loop(0, count // fine)
    def _(i):
        part = pl.ds(pl.multiple_of(i * fine, fine), fine)
        xf = normed[part, :].astype(jnp.float32)
        scale = lax.rsqrt(jnp.mean(xf * xf, axis=-1, keepdims=True) + 1e-06)
        normed[part, :] = (xf * scale * gain[...]).astype(jnp.bfloat16)

    loads[1].wait()
    loads[2].wait()

    def accumulate(step):
        og, ou = owner(0, step), owner(1, step)

        @pl.loop(0, count // tile)
        def _(i):
            part = pl.ds(pl.multiple_of(i * tile, tile), tile)
            for o, buf, acc in ((og, gbuf, gacc), (ou, ubuf, uacc)):
                a = normed[part, pl.ds(pl.multiple_of(o * rows, rows), rows)]
                if step == 0:
                    acc[part, :] = dot(a, buf[o])
                else:
                    acc[part, :] += dot(a, buf[o])

    base = 2 * (n - 1)
    for step in range(1, n):
        for c in range(2):
            for way, (own, buf) in enumerate(first):
                arrive(way, buf, step, c, 2 * (step - 1) + c)
                if step < n - 1:
                    go(hop(way, own, buf, step, c, 2 * step + c))
            if c == 0:
                accumulate(step - 1)
        if step == n - 2:
            for c in range(2):
                for way in range(2):
                    go(hop(way, dw, dbuf, 0, c, base + c))
    accumulate(n - 1)

    @pl.loop(0, count // fine)
    def _(i):
        part = pl.ds(pl.multiple_of(i * fine, fine), fine)
        v = gacc[part, :]
        hidden[part, :] = (v / (1.0 + jnp.exp(-v)) * uacc[part, :]).astype(jnp.bfloat16)

    loads[3].wait()
    shared = []
    whole = pl.ds(0, wide)
    cuts = splits_of(wide)
    narrow = [pl.ds(v * (wide // cuts), wide // cuts) for v in range(cuts)]

    def kept(index):
        return pl.ds(pl.multiple_of(index * keep, keep), keep)

    def share(o, cols=whole):
        @pl.loop(0, count // tile)
        def _(i):
            part = pl.ds(pl.multiple_of(i * tile, tile), tile)
            terms[o, part, cols] = dot(hidden[part, :], dbuf[o, :, cols]).astype(jnp.bfloat16)

        copies = []
        for k in range(chips):
            to = lax.rem(chip + 1 + k, chips)
            copy = pltpu.make_async_remote_copy(
                src_ref=terms.at[o, kept(2 * to + 1 - core), cols],
                dst_ref=paired.at[o, k, :, cols],
                send_sem=pair_send.at[len(shared), k],
                recv_sem=pair_recv.at[len(shared), k],
                device_id={"tp": partner},
                device_id_type=MESH,
            )
            go(copy)
            copies.append(copy)
        shared.append([o, copies, None, cols])

    def cross(j):
        o, pairs, unused, cols = shared[j]
        copies = []
        for k, other in enumerate(others):
            pairs[k].wait_recv()
            total = terms[o, kept(2 * other + core), cols].astype(jnp.float32) + paired[o, k, :, cols].astype(jnp.float32)
            summed[o, k, :, cols] = total.astype(jnp.bfloat16)
            copy = pltpu.make_async_remote_copy(
                src_ref=summed.at[o, k, :, cols],
                dst_ref=got.at[k, o, :, cols],
                send_sem=rs_send.at[j, k],
                recv_sem=rs_recv.at[j, k],
                device_id={"tp": 2 * other + core},
                device_id_type=MESH,
            )
            go(copy)
            copies.append(copy)
        shared[j][2] = copies

    last = n // 2 - 1
    for step in range(1, n // 2):
        for c in range(2):
            for way in range(2):
                arrive(way, dbuf, step, c, base + 2 * (step - 1) + c)
                if step < last:
                    go(hop(way, dw, dbuf, step, c, base + 2 * step + c))
                elif c == way:
                    for v, cols in enumerate(narrow):
                        go(hop(way, dw, dbuf, step, c, base + 2 * last + v, cols))
            if step == 1 and c == 0:
                share(me)
                cross(0)
        share(owner(0, step))
        share(owner(1, step))
        cross(2 * step - 1)
        cross(2 * step)
    for v, cols in enumerate(narrow):
        for way in range(2):
            arrive(way, dbuf, n // 2, way, base + 2 * last + v, cols)
        share(owner(0, n // 2), cols)
        cross(n - 1 + v)

    for o, pairs, copies, cols in shared:
        pairs[chips - 1].wait_recv()
        for copy in copies:
            copy.wait_recv()
        total = terms[o, kept(mine), cols].astype(jnp.float32) + paired[o, chips - 1, :, cols].astype(jnp.float32)
        for k in range(chips - 1):
            total = total + got[k, o, :, cols].astype(jnp.float32)
        out[:, pl.ds(pl.multiple_of(o * wide + cols.start, cols.size), cols.size)] = total.astype(out.dtype)
    for copy in sends:
        copy.wait_send()


def make_per_device(n, n_tp):
    def per_device(tokens, norm_gain, gate_weight, up_weight, down_weight):
        count, width = tokens.shape
        units = gate_weight.shape[1]
        wide = down_weight.shape[1]
        keep = count // n_tp
        bf16, f32 = jnp.bfloat16, jnp.float32
        cuts = splits_of(wide)
        events = 2 * (n - 1) + 2 * (n // 2 - 1) + cuts
        flops = 6 * count * width * units
        any_ref = pl.BlockSpec(memory_space=pl.ANY)
        vmem_ref = pl.BlockSpec(memory_space=pltpu.VMEM)
        return pl.pallas_call(
            functools.partial(kernel, n, n_tp),
            out_shape=jax.ShapeDtypeStruct((keep, width), bf16),
            in_specs=[any_ref, vmem_ref, any_ref, any_ref, any_ref],
            out_specs=vmem_ref,
            scratch_shapes=[
                pltpu.VMEM((count, width), bf16),
                pltpu.VMEM((count, units), f32),
                pltpu.VMEM((count, units), f32),
                pltpu.VMEM((count, units), bf16),
                pltpu.VMEM((n,) + gate_weight.shape, bf16),
                pltpu.VMEM((n,) + up_weight.shape, bf16),
                pltpu.VMEM((n,) + down_weight.shape, bf16),
                pltpu.VMEM((n, count, wide), bf16),
                pltpu.VMEM((n, n_tp // 2, keep, wide), bf16),
                pltpu.VMEM((n, n_tp // 2 - 1, keep, wide), bf16),
                pltpu.VMEM((n_tp // 2 - 1, n, keep, wide), bf16),
                pltpu.SemaphoreType.DMA((2, events)),
                pltpu.SemaphoreType.DMA((2, events)),
                pltpu.SemaphoreType.DMA((n - 1 + cuts, n_tp // 2)),
                pltpu.SemaphoreType.DMA((n - 1 + cuts, n_tp // 2)),
                pltpu.SemaphoreType.DMA((n - 1 + cuts, n_tp // 2 - 1)),
                pltpu.SemaphoreType.DMA((n - 1 + cuts, n_tp // 2 - 1)),
                pltpu.SemaphoreType.DMA((4,)),
            ],
            compiler_params=pltpu.CompilerParams(
                collective_id=0, has_side_effects=True, vmem_limit_bytes=66_000_000
            ),
            cost_estimate=pl.CostEstimate(flops=flops, bytes_accessed=2 * count * width, transcendentals=count * units),
        )(tokens, norm_gain.reshape(1, width), gate_weight, up_weight, down_weight)

    return per_device


def solution(mesh):
    placed = (P("fs", None), P(), P("fs", "tp"), P("fs", "tp"), P("tp", "fs"))
    return jax.shard_map(
        make_per_device(mesh.shape["fs"], mesh.shape["tp"]),
        mesh=mesh, in_specs=placed, out_specs=P(("fs", "tp"), None), check_vma=False,
    )
```

```python
import functools

import jax
import jax.numpy as jnp
from jax import lax
from jax.experimental import pallas as pl
from jax.experimental.pallas import tpu as pltpu
from jax.sharding import PartitionSpec as P

MESH = pl.DeviceIdType.MESH


def grid_of(n):
    ny = 2
    while ny * ny * 4 <= n:
        ny *= 2
    return n // ny, ny


def fs_of(place, n):
    nz, ny = grid_of(n)
    on = lax.div(place + (n - ny), n)
    rest = (place - ny) * on
    y, r = lax.div(rest, nz - 1), lax.rem(rest, nz - 1)
    odd = lax.rem(y, 2)
    z = 1 + (1 - odd) * r + odd * (nz - 2 - r)
    return on * (z * ny + y) + (1 - on) * (ny - 1 - place)


def place_of(fs, n):
    nz, ny = grid_of(n)
    z, y = lax.div(fs, ny), lax.rem(fs, ny)
    on = lax.div(z + nz - 1, nz)
    up = (z - 1) * on
    odd = lax.rem(y, 2)
    r = (1 - odd) * up + odd * (nz - 2 - up)
    return on * (ny + y * (nz - 1) + r) + (1 - on) * (ny - 1 - y)


def splits_of(wide):
    return 2 if wide % 256 == 0 else 1


def dot(a, b):
    return jnp.dot(a, b, preferred_element_type=jnp.float32)


def kernel(n, n_tp, tokens, gain, gw, uw, dw, out, normed, gacc, uacc, hidden, gbuf, ubuf, dbuf, terms, paired, summed,
           got, send, recv, pair_send, pair_recv, rs_send, rs_recv, local):
    me, mine = lax.axis_index("fs"), lax.axis_index("tp")
    at = place_of(me, n)
    neighbour = [fs_of(lax.rem(at + 1, n), n), fs_of(lax.rem(at + n - 1, n), n)]
    wide = dw.shape[1]
    rows = gw.shape[0]
    keep = out.shape[0]
    count = normed.shape[0]
    tile = 256

    def owner(way, step):
        step = step if way == 0 else n - step
        return fs_of(lax.rem(at + n - step, n), n)

    barrier = pltpu.get_barrier_semaphore()
    for way in range(2):
        pl.semaphore_signal(barrier, inc=1, device_id={"fs": neighbour[way]}, device_id_type=MESH)
    chips = n_tp // 2
    core, chip = lax.rem(mine, 2), lax.div(mine, 2)
    partner = 2 * chip + 1 - core
    others = [lax.rem(chip + k, chips) for k in range(1, chips)]
    for peer in [partner] + [2 * other + core for other in others]:
        pl.semaphore_signal(barrier, inc=1, device_id={"tp": peer}, device_id_type=MESH)

    loads = [
        pltpu.make_async_copy(tokens, normed, local.at[0]),
        pltpu.make_async_copy(gw, gbuf.at[me], local.at[1]),
        pltpu.make_async_copy(uw, ubuf.at[me], local.at[2]),
        pltpu.make_async_copy(dw, dbuf.at[me], local.at[3]),
    ]
    for load in loads:
        load.start()
    pl.semaphore_wait(barrier, 2 + chips)

    def hop(way, own, buf, step, c, event, cols=None):
        half = own.shape[0] // 2
        part = (pl.ds(c * half, half),) + (() if cols is None else (cols,))
        o = owner(way, step)
        return pltpu.make_async_remote_copy(
            src_ref=own.at[part] if step == 0 else buf.at[(o,) + part],
            dst_ref=buf.at[(o,) + part],
            send_sem=send.at[way, event],
            recv_sem=recv.at[way, event],
            device_id={"fs": neighbour[way]},
            device_id_type=MESH,
        )

    def arrive(way, buf, step, c, event, cols=None):
        half = buf.shape[1] // 2
        part = (pl.ds(c * half, half),) + (() if cols is None else (cols,))
        here = buf.at[(owner(way, step),) + part]
        pltpu.make_async_remote_copy(
            src_ref=here, dst_ref=here, send_sem=send.at[way, event], recv_sem=recv.at[way, event],
            device_id={"fs": neighbour[way]}, device_id_type=MESH,
        ).wait_recv()

    sends = []

    def go(copy):
        copy.start()
        sends.append(copy)

    first = [(gw, gbuf), (uw, ubuf)]
    for c in range(2):
        for way, (own, buf) in enumerate(first):
            go(hop(way, own, buf, 0, c, c))

    loads[0].wait()
    fine = 32

    @pl.loop(0, count // fine)
    def _(i):
        part = pl.ds(pl.multiple_of(i * fine, fine), fine)
        xf = normed[part, :].astype(jnp.float32)
        scale = lax.rsqrt(jnp.mean(xf * xf, axis=-1, keepdims=True) + 1e-06)
        normed[part, :] = (xf * scale * gain[...]).astype(jnp.bfloat16)

    loads[1].wait()
    loads[2].wait()

    def accumulate(step):
        og, ou = owner(0, step), owner(1, step)

        @pl.loop(0, count // tile)
        def _(i):
            part = pl.ds(pl.multiple_of(i * tile, tile), tile)
            for o, buf, acc in ((og, gbuf, gacc), (ou, ubuf, uacc)):
                a = normed[part, pl.ds(pl.multiple_of(o * rows, rows), rows)]
                if step == 0:
                    acc[part, :] = dot(a, buf[o])
                else:
                    acc[part, :] += dot(a, buf[o])

    base = 2 * (n - 1)
    for step in range(1, n):
        for c in range(2):
            for way, (own, buf) in enumerate(first):
                arrive(way, buf, step, c, 2 * (step - 1) + c)
                if step < n - 1:
                    go(hop(way, own, buf, step, c, 2 * step + c))
            if c == 0:
                accumulate(step - 1)
        if step == n - 2:
            for c in range(2):
                for way in range(2):
                    go(hop(way, dw, dbuf, 0, c ^ way, base + c))
    accumulate(n - 1)

    @pl.loop(0, count // fine)
    def _(i):
        part = pl.ds(pl.multiple_of(i * fine, fine), fine)
        v = gacc[part, :]
        hidden[part, :] = (v / (1.0 + jnp.exp(-v)) * uacc[part, :]).astype(jnp.bfloat16)

    loads[3].wait()
    shared = []
    whole = pl.ds(0, wide)
    cuts = splits_of(wide)
    narrow = [pl.ds(v * (wide // cuts), wide // cuts) for v in range(cuts)]

    def kept(index):
        return pl.ds(pl.multiple_of(index * keep, keep), keep)

    def share(o, cols=whole):
        @pl.loop(0, count // tile)
        def _(i):
            part = pl.ds(pl.multiple_of(i * tile, tile), tile)
            terms[o, part, cols] = dot(hidden[part, :], dbuf[o, :, cols]).astype(jnp.bfloat16)

        copies = []
        for k in range(chips):
            to = lax.rem(chip + 1 + k, chips)
            copy = pltpu.make_async_remote_copy(
                src_ref=terms.at[o, kept(2 * to + 1 - core), cols],
                dst_ref=paired.at[o, k, :, cols],
                send_sem=pair_send.at[len(shared), k],
                recv_sem=pair_recv.at[len(shared), k],
                device_id={"tp": partner},
                device_id_type=MESH,
            )
            go(copy)
            copies.append(copy)
        shared.append([o, copies, None, cols])

    def cross(j):
        o, pairs, unused, cols = shared[j]
        copies = []
        for k, other in enumerate(others):
            pairs[k].wait_recv()
            total = terms[o, kept(2 * other + core), cols].astype(jnp.float32) + paired[o, k, :, cols].astype(jnp.float32)
            summed[o, k, :, cols] = total.astype(jnp.bfloat16)
            copy = pltpu.make_async_remote_copy(
                src_ref=summed.at[o, k, :, cols],
                dst_ref=got.at[k, o, :, cols],
                send_sem=rs_send.at[j, k],
                recv_sem=rs_recv.at[j, k],
                device_id={"tp": 2 * other + core},
                device_id_type=MESH,
            )
            go(copy)
            copies.append(copy)
        shared[j][2] = copies

    last = n // 2 - 1
    for step in range(1, n // 2):
        for c in range(2):
            for way in range(2):
                arrive(way, dbuf, step, c ^ way, base + 2 * (step - 1) + c)
                if step < last:
                    go(hop(way, dw, dbuf, step, c ^ way, base + 2 * step + c))
                elif c == 0:
                    for v, cols in enumerate(narrow):
                        go(hop(way, dw, dbuf, step, way, base + 2 * last + v, cols))
            if step == 1 and c == 0:
                share(me)
                cross(0)
        share(owner(0, step))
        share(owner(1, step))
        cross(2 * step - 1)
        cross(2 * step)
    for v, cols in enumerate(narrow):
        for way in range(2):
            arrive(way, dbuf, n // 2, way, base + 2 * last + v, cols)
        share(owner(0, n // 2), cols)
        cross(n - 1 + v)

    for o, pairs, copies, cols in shared:
        pairs[chips - 1].wait_recv()
        for copy in copies:
            copy.wait_recv()
        total = terms[o, kept(mine), cols].astype(jnp.float32) + paired[o, chips - 1, :, cols].astype(jnp.float32)
        for k in range(chips - 1):
            total = total + got[k, o, :, cols].astype(jnp.float32)
        out[:, pl.ds(pl.multiple_of(o * wide + cols.start, cols.size), cols.size)] = total.astype(out.dtype)
    for copy in sends:
        copy.wait_send()


def make_per_device(n, n_tp):
    def per_device(tokens, norm_gain, gate_weight, up_weight, down_weight):
        count, width = tokens.shape
        units = gate_weight.shape[1]
        wide = down_weight.shape[1]
        keep = count // n_tp
        bf16, f32 = jnp.bfloat16, jnp.float32
        cuts = splits_of(wide)
        events = 2 * (n - 1) + 2 * (n // 2 - 1) + cuts
        flops = 6 * count * width * units
        any_ref = pl.BlockSpec(memory_space=pl.ANY)
        vmem_ref = pl.BlockSpec(memory_space=pltpu.VMEM)
        return pl.pallas_call(
            functools.partial(kernel, n, n_tp),
            out_shape=jax.ShapeDtypeStruct((keep, width), bf16),
            in_specs=[any_ref, vmem_ref, any_ref, any_ref, any_ref],
            out_specs=vmem_ref,
            scratch_shapes=[
                pltpu.VMEM((count, width), bf16),
                pltpu.VMEM((count, units), f32),
                pltpu.VMEM((count, units), f32),
                pltpu.VMEM((count, units), bf16),
                pltpu.VMEM((n,) + gate_weight.shape, bf16),
                pltpu.VMEM((n,) + up_weight.shape, bf16),
                pltpu.VMEM((n,) + down_weight.shape, bf16),
                pltpu.VMEM((n, count, wide), bf16),
                pltpu.VMEM((n, n_tp // 2, keep, wide), bf16),
                pltpu.VMEM((n, n_tp // 2 - 1, keep, wide), bf16),
                pltpu.VMEM((n_tp // 2 - 1, n, keep, wide), bf16),
                pltpu.SemaphoreType.DMA((2, events)),
                pltpu.SemaphoreType.DMA((2, events)),
                pltpu.SemaphoreType.DMA((n - 1 + cuts, n_tp // 2)),
                pltpu.SemaphoreType.DMA((n - 1 + cuts, n_tp // 2)),
                pltpu.SemaphoreType.DMA((n - 1 + cuts, n_tp // 2 - 1)),
                pltpu.SemaphoreType.DMA((n - 1 + cuts, n_tp // 2 - 1)),
                pltpu.SemaphoreType.DMA((4,)),
            ],
            compiler_params=pltpu.CompilerParams(
                collective_id=0, has_side_effects=True, vmem_limit_bytes=66_000_000
            ),
            cost_estimate=pl.CostEstimate(flops=flops, bytes_accessed=2 * count * width, transcendentals=count * units),
        )(tokens, norm_gain.reshape(1, width), gate_weight, up_weight, down_weight)

    return per_device


def solution(mesh):
    placed = (P("fs", None), P(), P("fs", "tp"), P("fs", "tp"), P("tp", "fs"))
    return jax.shard_map(
        make_per_device(mesh.shape["fs"], mesh.shape["tp"]),
        mesh=mesh, in_specs=placed, out_specs=P(("fs", "tp"), None), check_vma=False,
    )
```
